32 devices in a mesh: sp: 8 (over z, x), tp: 4 (over y, core).
Axes of the slice: x: 2, y: 2, z: 4, core: 2. Of those that a mesh axis runs over, the one named last changes fastest.
Arguments:
- tokens: bfloat16 [2048, 2048], P('sp', 'tp'), may hold values from -6 to 6
- segments: int32 [2048], P('sp'), may hold values from 0 to 3, never falling along the last dimension, each value on 1 to 1024 neighbouring positions
- in_gain: float32 [2, 2048], replicated, may hold values from 0.1 to 1.9
- w_value: bfloat16 [2, 2048, 1024], P(None, 'sp', 'tp'), may hold values from -0.125 to 0.125
- w_gate: bfloat16 [2, 2048, 1024], P(None, 'sp', 'tp'), may hold values from -0.125 to 0.125
- conv_taps: float32 [2, 129, 1024], P(None, None, 'tp'), may hold values from -4 to 4, as said below
- norm_gain: float32 [2, 1024], P(None, 'tp'), may hold values from 0.1 to 1.9
- w_out: bfloat16 [2, 1024, 2048], P(None, 'tp', 'sp'), may hold values from -0.1875 to 0.1875
Outputs:
- mixed: bfloat16 [2048, 2048], P('sp', 'tp')
The draws below stay inside these ranges and needn't reach their ends.
Inputs may be any that keep to these rules, and one draw needn't show every extreme that they name: `segments`: document numbers never fall along the sequence; each document has 1 to 1024 positions, one has exactly 1024. `conv_taps`: real-valued taps.
All inputs are finite; a program needn't handle non-finite values.
Results may differ from the reference program's by a relative error of at most 0.014.
Values may be sent and summed in bfloat16 or wider, within the bound.
A program may use at most 64 MiB of HBM per device.

```python
import math
import jax
import jax.numpy as jnp
import numpy as np
from jax import lax

D = 2048
CF = 1024
KW = 129
LAYERS = 2
TOKENS = 2048
CF_DEV = 256
DOCS = 4
DOC_MOST = 1024
N_TP = 4


def draw_conv_taps(key, part):
    first, second = jax.random.split(key, 2)
    group_scale = jnp.exp(jax.random.uniform(first, (8,), jnp.float32, jnp.log(0.3), jnp.log(3.0)))
    channel_scale = jnp.repeat(group_scale, CF // 8)
    base = jnp.clip(jax.random.normal(second, (LAYERS, KW, CF), jnp.float32), -4.0, 4.0)
    return (base * channel_scale * KW ** (-0.5)).astype(jnp.float32)


def block_scale(stream_key, extent, cuts, low, high):
    level, own = 1.0, jax.random.fold_in(stream_key, 6)
    for dim, parts in cuts:
        heights = jnp.exp(jax.random.uniform(jax.random.fold_in(own, dim), (parts,), jnp.float32, low / len(cuts), high / len(cuts)))
        level = level * jnp.repeat(heights, extent[dim] // parts).reshape([-1 if axis == dim else 1 for axis in range(len(extent))])
    return level


def length_profile(number_of, total, bound, lean):
    weights = [(1 << 20) // math.isqrt(grade ** lean) + 1 for grade in range(2, number_of + 1)]
    rest, given = total - bound - (number_of - 1), [1] * (number_of - 1)
    while rest > 0:
        candidates = [i for i in range(number_of - 1) if given[i] < bound]
        whole, remaining = sum([weights[i] for i in candidates]), rest
        for i in candidates:
            more = min(bound - given[i], max(1, remaining * weights[i] // whole), rest)
            given[i] = given[i] + more
            rest = rest - more
    return np.array([bound] + given)


def ragged(own_key, number_of, total, most, slope):
    if number_of == 2:
        one = jax.random.randint(own_key, (), max(1, total - most), min(most, total - 1) + 1)
        return jnp.stack([one, total - one])
    lengths = jnp.asarray(length_profile(number_of, total, most, slope), jnp.int32)
    couples = (number_of - 1) // 2
    giver, taker = lengths[1:1 + 2 * couples:2], lengths[2:2 + 2 * couples:2]
    margin = jnp.minimum(giver - 1, most - taker)
    moved = jax.random.randint(jax.random.fold_in(own_key, 1), (couples,), 0, 1 << 20) % (margin + 1)
    lengths = lengths.at[1:1 + 2 * couples:2].set(giver - moved).at[2:2 + 2 * couples:2].set(taker + moved)
    return lengths[jax.random.permutation(jax.random.fold_in(own_key, 2), number_of)]


def bell_draw(rng, extent, spread, reach, shards=(), dtype=jnp.bfloat16):
    drawn = spread * jax.random.normal(rng, extent, jnp.float32)
    if shards:
        drawn = drawn * block_scale(rng, extent, shards, -0.22, 0.18)
    return jnp.clip(drawn, -reach, reach).astype(dtype)


def setup_inputs(seed: int = 0) -> dict:
    arg_keys = jax.random.split(jax.random.key(seed), 9)
    tokens = bell_draw(arg_keys[0], (TOKENS, D), 1.0, 6.0, ((0, 8), (1, 4)))
    segments = jnp.searchsorted(jnp.cumsum(ragged(arg_keys[1], DOCS, TOKENS, DOC_MOST, 2)), jnp.arange(TOKENS), side="right").astype(jnp.int32)
    in_gain = jnp.clip(1.0 + 0.18 * jax.random.normal(arg_keys[2], (LAYERS, D), jnp.float32), 0.1, 1.9)
    w_value = bell_draw(arg_keys[3], (LAYERS, D, CF), D ** -0.5, 0.125, ((1, 8), (2, 4)))
    w_gate = bell_draw(arg_keys[4], (LAYERS, D, CF), D ** -0.5, 0.125, ((1, 8), (2, 4)))
    conv_taps = draw_conv_taps(jax.random.fold_in(arg_keys[8], 71), 0)
    norm_gain = jnp.clip(1.0 + 0.18 * jax.random.normal(arg_keys[6], (LAYERS, CF), jnp.float32), 0.1, 1.9)
    w_out = bell_draw(arg_keys[7], (LAYERS, CF, D), CF ** -0.5, 0.1875, ((1, 4), (2, 8)))
    return {"tokens": tokens, "segments": segments, "in_gain": in_gain, "w_value": w_value, "w_gate": w_gate, "conv_taps": conv_taps, "norm_gain": norm_gain, "w_out": w_out}


EPSILON = 0.01

def rms_rows(stream, gain):
    wide_vals = stream.astype(jnp.float32)
    scale = lax.rsqrt(lax.optimization_barrier(jnp.mean(wide_vals * wide_vals, axis=-1, keepdims=True)) + EPSILON)
    return (wide_vals * scale * gain).astype(jnp.bfloat16)

def reference(tokens, segments, in_gain, w_value, w_gate, conv_taps, norm_gain, w_out):
    fringe = (KW - 1) // 2
    seg_pad = jnp.pad(segments, (fringe, fringe), constant_values=-1)
    stream = tokens
    for layer_idx in range(LAYERS):
        normed = rms_rows(stream, in_gain[layer_idx])
        value_pre = jnp.dot(normed, w_value[layer_idx], preferred_element_type=jnp.float32)
        gate_pre = jnp.dot(normed, w_gate[layer_idx], preferred_element_type=jnp.float32)
        gated = (value_pre * jax.nn.sigmoid(gate_pre)).astype(jnp.bfloat16)
        padded = jnp.pad(gated.astype(jnp.float32), ((fringe, fringe), (0, 0)))
        tap_table = conv_taps[layer_idx]

        def add_tap(shift_idx, running):
            shift_idx = jnp.asarray(shift_idx).astype(jnp.int32)
            window = lax.dynamic_slice_in_dim(padded, shift_idx, TOKENS, 0)
            same_doc = lax.dynamic_slice_in_dim(seg_pad, shift_idx, TOKENS, 0) == segments
            tap_row = lax.dynamic_slice_in_dim(tap_table, shift_idx, 1, 0)
            return running + jnp.where(same_doc[:, None], window * tap_row, jnp.float32(0.0))
        conv = lax.fori_loop(0, KW, add_tap, jnp.zeros((TOKENS, CF), jnp.float32))
        row_mean = lax.optimization_barrier(jnp.mean(conv, axis=-1, keepdims=True))
        centred = conv - row_mean
        row_var = lax.optimization_barrier(jnp.mean(centred * centred, axis=-1, keepdims=True))
        activated = jax.nn.silu(centred * lax.rsqrt(row_var + EPSILON) * norm_gain[layer_idx]).astype(jnp.bfloat16)
        out_weight = w_out[layer_idx]

        def add_block(block_idx, running):
            first = (jnp.asarray(block_idx) * CF_DEV).astype(jnp.int32)
            columns = lax.dynamic_slice_in_dim(activated, first, CF_DEV, 1)
            weight_rows = lax.dynamic_slice_in_dim(out_weight, first, CF_DEV, 0)
            partial_value = jnp.dot(columns, weight_rows, preferred_element_type=jnp.float32)
            return running + lax.optimization_barrier(partial_value.astype(jnp.bfloat16)).astype(jnp.float32)
        summed = lax.fori_loop(0, N_TP, add_block, jnp.zeros((TOKENS, D), jnp.float32))
        stream = (stream.astype(jnp.float32) + summed).astype(jnp.bfloat16)
    return stream
```

```python
import functools

import jax
import jax.numpy as jnp
from jax import lax
from jax.experimental import pallas as pl
from jax.experimental.pallas import tpu as pltpu
from jax.sharding import PartitionSpec as P

EPSILON = 0.01
LANES = 128
PAIR = 2
RELAY_MOST = 8
F32 = jnp.float32
BF16 = jnp.bfloat16
MESH = pl.DeviceIdType.MESH


def remote(src, dst, send, recv, axis, index):
    return pltpu.make_async_remote_copy(
        src_ref=src,
        dst_ref=dst,
        send_sem=send,
        recv_sem=recv,
        device_id={axis: index},
        device_id_type=MESH,
    )


def kernel(
    cfg, tok, seg, gain_in, wv, wg, wo, taps, gain_norm, out,
    stream, normed, gvg, gout, xbuf, segw, conv, act, stat, part, first, pair, far, own,
    w_recv, w_send_z, w_send_x, tok_recv, tok_send, sib_send, seg_send, seg_recv,
    halo_send, halo_recv, stat_send, stat_recv, first_send, first_recv,
    far_send, far_recv, fin_recv, fin_send,
):
    n_sp, n_tp, layers, kw, gather = cfg
    fringe = (kw - 1) // 2
    rows, width = tok.shape
    tiles = xbuf.shape[1]
    chan = tiles * LANES
    line, half = n_sp // PAIR, n_tp // PAIR
    s, t = lax.axis_index("sp"), lax.axis_index("tp")
    z, x = s // PAIR, lax.rem(s, PAIR)
    h, c = t // PAIR, lax.rem(t, PAIR)
    x_next = z * PAIR + (1 - x)
    sib = h * PAIR + (1 - c)

    barrier = pltpu.get_barrier_semaphore()
    greeted = range(1, n_sp) if gather else (1, n_sp - 1)
    for d in greeted:
        pl.semaphore_signal(barrier, inc=1, device_id={"sp": lax.rem(s + d, n_sp)}, device_id_type=MESH)
    for d in range(1, n_tp):
        pl.semaphore_signal(barrier, inc=1, device_id={"tp": lax.rem(t + d, n_tp)}, device_id_type=MESH)
    pl.semaphore_wait(barrier, len(greeted) + n_tp - 1)

    sends = []

    def go(copy):
        copy.start()
        sends.append(copy)

    def slot(layer, mat, origin):
        return gout.at[layer, origin] if mat == 2 else gvg.at[layer, mat, origin]

    def local(layer, mat):
        return (wv, wg, wo)[mat].at[layer]

    def send_own(layer, mat):
        if not gather:
            return
        p = layer * 3 + mat
        for d in range(1, line):
            go(remote(local(layer, mat), slot(layer, mat, s), w_send_z.at[p, d], w_recv.at[p, s], "sp",
                      lax.rem(z + d, line) * PAIR + x))
        go(remote(local(layer, mat), slot(layer, mat, s), w_send_x.at[p, 0], w_recv.at[p, s], "sp", x_next))
        slot(layer, mat, s)[...] = local(layer, mat)[...]

    def arrived(layer, mat, origin):
        p = layer * 3 + mat
        remote(local(layer, mat), slot(layer, mat, origin), w_send_x.at[p, 0], w_recv.at[p, origin], "sp", x_next).wait_recv()

    def relay(layer, mat):
        if not gather:
            return
        p = layer * 3 + mat
        for d in range(1, line):
            origin = lax.rem(z + line - d, line) * PAIR + x
            arrived(layer, mat, origin)
            block = slot(layer, mat, origin)
            go(remote(block, block, w_send_x.at[p, d], w_recv.at[p, origin], "sp", x_next))

    def settle(layer, mat):
        if not gather:
            return
        for d in range(line):
            arrived(layer, mat, lax.rem(z + line - d, line) * PAIR + (1 - x))

    def both_sides(make, count):
        for i in range(count):
            @pl.when(s > 0)
            def _():
                make(i, 0).start()

            @pl.when(s < n_sp - 1)
            def _():
                make(i, 1).start()

    def both_wait(make, count):
        for i in range(count):
            @pl.when(s > 0)
            def _():
                make(i, 0).wait_send()
                make(i, 1).wait_recv()

            @pl.when(s < n_sp - 1)
            def _():
                make(i, 1).wait_send()
                make(i, 0).wait_recv()

    def seg_copy(i, side):
        src = segw.at[pl.ds(fringe, fringe)] if side == 0 else segw.at[pl.ds(rows, fringe)]
        dst = segw.at[pl.ds(fringe + rows, fringe)] if side == 0 else segw.at[pl.ds(0, fringe)]
        return remote(src, dst, seg_send.at[side], seg_recv.at[side], "sp",
                      jnp.maximum(s - 1, 0) if side == 0 else jnp.minimum(s + 1, n_sp - 1))

    def halo_copy(layer):
        def make(i, side):
            buf = xbuf.at[layer, i]
            src = buf.at[pl.ds(fringe, fringe)] if side == 0 else buf.at[pl.ds(rows, fringe)]
            dst = buf.at[pl.ds(fringe + rows, fringe)] if side == 0 else buf.at[pl.ds(0, fringe)]
            return remote(src, dst, halo_send.at[layer, i, side], halo_recv.at[layer, i, side], "sp",
                          jnp.maximum(s - 1, 0) if side == 0 else jnp.minimum(s + 1, n_sp - 1))
        return make

    segw[pl.ds(fringe, rows)] = seg[...]

    @pl.when(s == 0)
    def _():
        segw[pl.ds(0, fringe)] = jnp.full((fringe, LANES), -1, jnp.int32)
        for layer in range(layers):
            for i in range(tiles):
                xbuf[layer, i, pl.ds(0, fringe)] = jnp.zeros((fringe, LANES), F32)

    @pl.when(s == n_sp - 1)
    def _():
        segw[pl.ds(fringe + rows, fringe)] = jnp.full((fringe, LANES), -1, jnp.int32)
        for layer in range(layers):
            for i in range(tiles):
                xbuf[layer, i, pl.ds(fringe + rows, fringe)] = jnp.zeros((fringe, LANES), F32)

    both_sides(seg_copy, 1)
    for mat in range(2):
        send_own(0, mat)
    for d in range(1, half):
        go(remote(tok, stream.at[0, t], tok_send.at[d], tok_recv.at[t], "tp", lax.rem(h + d, half) * PAIR + c))
    go(remote(tok, stream.at[0, t], sib_send.at[0, 0], tok_recv.at[t], "tp", sib))
    stream[0, t] = tok[...]
    relay(0, 0)
    for d in range(1, half):
        origin = lax.rem(h + half - d, half) * PAIR + c
        block = stream.at[0, origin]
        remote(tok, block, tok_send.at[d], tok_recv.at[origin], "tp", sib).wait_recv()
        go(remote(block, block, sib_send.at[0, d], tok_recv.at[origin], "tp", sib))
    relay(0, 1)
    for d in range(half):
        origin = lax.rem(h + half - d, half) * PAIR + (1 - c)
        remote(tok, stream.at[0, origin], sib_send.at[0, d], tok_recv.at[origin], "tp", sib).wait_recv()
    both_wait(seg_copy, 1)

    for layer in range(layers):
        last = layer == layers - 1

        def norm_step(i, _):
            at = pl.ds(pl.multiple_of(i * 32, 32), 32)
            total = jnp.zeros((32, 1), F32)
            for j in range(n_tp):
                v = stream[layer, j, at, :].astype(F32)
                total = total + jnp.sum(v * v, axis=-1, keepdims=True)
            scale = lax.rsqrt(total / (n_tp * width) + EPSILON)
            for j in range(n_tp):
                v = stream[layer, j, at, :].astype(F32)
                cut = slice(j * width, (j + 1) * width)
                normed[at, cut] = (v * scale * gain_in[layer : layer + 1, cut]).astype(BF16)
            return 0

        lax.fori_loop(0, rows // 32, norm_step, 0)
        settle(layer, 0)
        settle(layer, 1)

        def gate_step(i, _):
            at = pl.ds(pl.multiple_of(i * 128, 128), 128)
            a = normed[at, :]
            if gather:
                w_value = gvg[layer, 0].reshape(n_tp * width, chan)
                w_gate = gvg[layer, 1].reshape(n_tp * width, chan)
            else:
                w_value, w_gate = wv[layer], wg[layer]
            value = jnp.dot(a, w_value, preferred_element_type=F32)
            gate = jnp.dot(a, w_gate, preferred_element_type=F32)
            gated = (value * jax.nn.sigmoid(gate)).astype(BF16).astype(F32)
            to = pl.ds(pl.multiple_of(fringe + i * 128, 64), 128)
            for j in range(tiles):
                xbuf[layer, j, to, :] = gated[:, j * LANES : (j + 1) * LANES]
            return 0

        lax.fori_loop(0, rows // 128, gate_step, 0)
        halo = halo_copy(layer)
        both_sides(halo, tiles)
        both_wait(halo, tiles)
        send_own(layer, 2)
        if not last:
            send_own(layer + 1, 0)
            send_own(layer + 1, 1)

        def conv_step(i, _):
            base = pl.multiple_of(i * 32, 32)
            here = segw[pl.ds(base + fringe, 32), :]
            acc = [jnp.zeros((32, LANES), F32) for _ in range(tiles)]
            for k in range(kw):
                same = segw[pl.ds(base + k, 32), :] == here
                for j in range(tiles):
                    tap = taps[layer, k : k + 1, j * LANES : (j + 1) * LANES]
                    acc[j] = acc[j] + jnp.where(same, xbuf[layer, j, pl.ds(base + k, 32), :] * tap, 0.0)
            at = pl.ds(base, 32)
            total = sum(jnp.sum(a, axis=-1, keepdims=True) for a in acc)
            mean = total / chan
            square = sum(jnp.sum((a - mean) * (a - mean), axis=-1, keepdims=True) for a in acc)
            for j in range(tiles):
                conv[at, j * LANES : (j + 1) * LANES] = acc[j]
            lane = lax.broadcasted_iota(jnp.int32, (32, LANES), 1)
            part[at, :] = jnp.where(lane == 0, mean, square)
            return 0

        lax.fori_loop(0, rows // 32, conv_step, 0)

        stat[layer, t] = jnp.transpose(part[...])[:8]
        for d in range(1, n_tp):
            go(remote(stat.at[layer, t], stat.at[layer, t], stat_send.at[layer, d], stat_recv.at[layer, t], "tp", lax.rem(t + d, n_tp)))
        relay(layer, 2)
        for d in range(1, n_tp):
            origin = lax.rem(t + n_tp - d, n_tp)
            remote(stat.at[layer, t], stat.at[layer, origin], stat_send.at[layer, d], stat_recv.at[layer, origin], "tp", origin).wait_recv()
        means = [stat[layer, j][0:1] for j in range(n_tp)]
        mean = sum(means) / n_tp
        spread = sum(stat[layer, j][1:2] + chan * (means[j] - mean) * (means[j] - mean) for j in range(n_tp))
        scale = lax.rsqrt(spread / (n_tp * chan) + EPSILON)
        row = lax.broadcasted_iota(jnp.int32, (LANES, rows), 0)
        part[...] = jnp.transpose(jnp.where(row == 0, mean, scale))

        def act_step(i, _):
            at = pl.ds(pl.multiple_of(i * 32, 32), 32)
            both = part[at, :]
            v = (conv[at, :] - both[:, 0:1]) * both[:, 1:2] * gain_norm[layer : layer + 1, :]
            act[at, :] = (v / (1.0 + jnp.exp(-v))).astype(BF16)
            return 0

        lax.fori_loop(0, rows // 32, act_step, 0)
        settle(layer, 2)

        blocks = gout if gather else wo
        cols = blocks.shape[-1]
        each = width // cols

        def project(target, put):
            for i in range(each):
                w = blocks[layer, target * each + i]
                put(slice(i * cols, (i + 1) * cols), jnp.dot(act[...], w, preferred_element_type=F32))

        for k in range(half):
            def put_first(cut, v, k=k):
                first[layer, 0, k, :, cut] = v.astype(BF16)

            project(k * PAIR + (1 - c), put_first)
            go(remote(first.at[layer, 0, k], first.at[layer, 1, k], first_send.at[layer, k], first_recv.at[layer, k], "tp", sib))
        for k in range(half):
            def put_own(cut, v, k=k):
                own[k, :, cut] = v

            project(k * PAIR + c, put_own)
        for d in range(half):
            k = lax.rem(h + half - 1 - d, half) if last else d
            remote(first.at[layer, 0, k], first.at[layer, 1, k], first_send.at[layer, k], first_recv.at[layer, k], "tp", sib).wait_recv()
            pair[layer, k] = (own[k] + first[layer, 1, k].astype(F32)).astype(BF16)
            if last:
                @pl.when(k != h)
                def _():
                    remote(pair.at[layer, k], far.at[layer, h, 0], fin_send.at[k], fin_recv.at[h], "tp", k * PAIR + c).start()
            else:
                for e in range(1, half):
                    go(remote(pair.at[layer, k], far.at[layer, h, k], far_send.at[layer, e, k], far_recv.at[layer, h, k], "tp",
                              lax.rem(h + e, half) * PAIR + c))
        if last:
            far[layer, h, 0] = pair[layer, h]
            for e in range(1, half):
                k = lax.rem(h + e, half)
                remote(pair.at[layer, k], far.at[layer, k, 0], fin_send.at[k], fin_recv.at[k], "tp", sib).wait()
            total = sum(far[layer, g, 0].astype(F32) for g in range(half))
            out[...] = (stream[layer, t].astype(F32) + total).astype(BF16)
        else:
            for k in range(half):
                far[layer, h, k] = pair[layer, k]
            relay(layer + 1, 0)
            for k in range(half):
                for e in range(1, half):
                    g = lax.rem(h + e, half)
                    remote(pair.at[layer, k], far.at[layer, g, k], far_send.at[layer, e, k], far_recv.at[layer, g, k], "tp", sib).wait_recv()
                total = sum(far[layer, g, k].astype(F32) for g in range(half))
                block = stream.at[layer + 1, k * PAIR + c]
                block[...] = (stream[layer, k * PAIR + c].astype(F32) + total).astype(BF16)
                go(remote(block, block, sib_send.at[layer + 1, k], far_recv.at[layer, half, k], "tp", sib))
            relay(layer + 1, 1)
            for k in range(half):
                block = stream.at[layer + 1, k * PAIR + (1 - c)]
                remote(block, block, sib_send.at[layer + 1, k], far_recv.at[layer, half, k], "tp", sib).wait_recv()

    for copy in sends:
        copy.wait_send()


def per_device(n_sp, n_tp, tokens, segments, in_gain, w_value, w_gate, conv_taps, norm_gain, w_out):
    layers, kw, chan = conv_taps.shape
    rows, width = tokens.shape
    gather = n_sp <= RELAY_MOST and n_sp % PAIR == 0
    if not gather:
        w_value = lax.all_gather(w_value, "sp", axis=1, tiled=True)
        w_gate = lax.all_gather(w_gate, "sp", axis=1, tiled=True)
        w_out = lax.all_gather(w_out, "sp", axis=2, tiled=True)
        w_out = w_out.reshape(layers, chan, n_tp, width).transpose(0, 2, 1, 3)
    held = (layers, 2, n_sp) + w_value.shape[1:] if gather else (1, 1, 1, 16, LANES)
    held_out = (layers, n_sp) + w_out.shape[1:] if gather else (1, 1, 16, LANES)
    tiles, half, fringe = chan // LANES, n_tp // PAIR, (kw - 1) // 2
    wide = rows + 2 * fringe
    dma = pltpu.SemaphoreType.DMA
    line = max(n_sp // PAIR, 1) if gather else 1
    held_sp = n_sp if gather else 1
    vmem = pl.BlockSpec(memory_space=pltpu.VMEM)
    return pl.pallas_call(
        functools.partial(kernel, (n_sp, n_tp, layers, kw, gather)),
        out_shape=jax.ShapeDtypeStruct((rows, width), BF16),
        in_specs=[vmem] * 8,
        out_specs=vmem,
        scratch_shapes=[
            pltpu.VMEM((layers, n_tp, rows, width), BF16),
            pltpu.VMEM((rows, n_tp * width), BF16),
            pltpu.VMEM(held, BF16),
            pltpu.VMEM(held_out, BF16),
            pltpu.VMEM((layers, tiles, wide, LANES), F32),
            pltpu.VMEM((wide, LANES), jnp.int32),
            pltpu.VMEM((rows, chan), F32),
            pltpu.VMEM((rows, chan), BF16),
            pltpu.VMEM((layers, n_tp, 8, rows), F32),
            pltpu.VMEM((rows, LANES), F32),
            pltpu.VMEM((layers, 2, half, rows, width), BF16),
            pltpu.VMEM((layers, half, rows, width), BF16),
            pltpu.VMEM((layers, half, half, rows, width), BF16),
            pltpu.VMEM((half, rows, width), F32),
            dma((layers * 3, held_sp)),
            dma((layers * 3, line)),
            dma((layers * 3, line)),
            dma((n_tp,)),
            dma((half,)),
            dma((layers, half)),
            dma((2,)),
            dma((2,)),
            dma((layers, tiles, 2)),
            dma((layers, tiles, 2)),
            dma((layers, n_tp)),
            dma((layers, n_tp)),
            dma((layers, half)),
            dma((layers, half)),
            dma((layers, half, half)),
            dma((layers, half + 1, half)),
            dma((half,)),
            dma((half,)),
        ],
        compiler_params=pltpu.CompilerParams(
            collective_id=0, has_side_effects=True, vmem_limit_bytes=60000 * 1024
        ),
    )(
        tokens,
        jnp.broadcast_to(segments[:, None], (rows, LANES)),
        in_gain,
        w_value,
        w_gate,
        w_out,
        conv_taps,
        norm_gain,
    )


def solution(mesh):
    in_specs = (
        P("sp", "tp"),
        P("sp"),
        P(),
        P(None, "sp", "tp"),
        P(None, "sp", "tp"),
        P(None, None, "tp"),
        P(None, "tp"),
        P(None, "tp", "sp"),
    )
    return jax.shard_map(
        functools.partial(per_device, mesh.shape["sp"], mesh.shape["tp"]),
        mesh=mesh,
        in_specs=in_specs,
        out_specs=P("sp", "tp"),
        check_vma=False,
    )
```

```python
import functools

import jax
import jax.numpy as jnp
from jax import lax
from jax.experimental import pallas as pl
from jax.experimental.pallas import tpu as pltpu
from jax.sharding import PartitionSpec as P

EPSILON = 0.01
LANES = 128
PAIR = 2
RELAY_MOST = 8
F32 = jnp.float32
BF16 = jnp.bfloat16
MESH = pl.DeviceIdType.MESH


def remote(src, dst, send, recv, axis, index):
    return pltpu.make_async_remote_copy(
        src_ref=src,
        dst_ref=dst,
        send_sem=send,
        recv_sem=recv,
        device_id={axis: index},
        device_id_type=MESH,
    )


def kernel(
    cfg, tok, seg, gain_in, wv, wg, wo, taps, gain_norm, out,
    stream, normed, gvg, gout, xbuf, segw, conv, act, stat, part, first, pair, far, own,
    w_recv, w_send_z, w_send_x, tok_recv, tok_send, sib_send, seg_send, seg_recv,
    halo_send, halo_recv, stat_send, stat_recv, first_send, first_recv,
    far_send, far_recv, fin_recv, fin_send,
):
    n_sp, n_tp, layers, kw, gather = cfg
    fringe = (kw - 1) // 2
    rows, width = tok.shape
    tiles = xbuf.shape[1]
    chan = tiles * LANES
    line, half = n_sp // PAIR, n_tp // PAIR
    s, t = lax.axis_index("sp"), lax.axis_index("tp")
    z, x = s // PAIR, lax.rem(s, PAIR)
    h, c = t // PAIR, lax.rem(t, PAIR)
    x_next = z * PAIR + (1 - x)
    sib = h * PAIR + (1 - c)

    barrier = pltpu.get_barrier_semaphore()
    greeted = range(1, n_sp) if gather else (1, n_sp - 1)
    for d in greeted:
        pl.semaphore_signal(barrier, inc=1, device_id={"sp": lax.rem(s + d, n_sp)}, device_id_type=MESH)
    for d in range(1, n_tp):
        pl.semaphore_signal(barrier, inc=1, device_id={"tp": lax.rem(t + d, n_tp)}, device_id_type=MESH)
    pl.semaphore_wait(barrier, len(greeted) + n_tp - 1)

    sends = []

    def go(copy):
        copy.start()
        sends.append(copy)

    def slot(layer, mat, origin):
        return gout.at[layer, origin] if mat == 2 else gvg.at[layer, mat, origin]

    def local(layer, mat):
        return (wv, wg, wo)[mat].at[layer]

    def send_own(layer, mat):
        if not gather:
            return
        p = layer * 3 + mat
        for d in range(1, line):
            go(remote(local(layer, mat), slot(layer, mat, s), w_send_z.at[p, d], w_recv.at[p, s], "sp",
                      lax.rem(z + d, line) * PAIR + x))
        go(remote(local(layer, mat), slot(layer, mat, s), w_send_x.at[p, 0], w_recv.at[p, s], "sp", x_next))
        slot(layer, mat, s)[...] = local(layer, mat)[...]

    def arrived(layer, mat, origin):
        p = layer * 3 + mat
        remote(local(layer, mat), slot(layer, mat, origin), w_send_x.at[p, 0], w_recv.at[p, origin], "sp", x_next).wait_recv()

    def relay(layer, mat):
        if not gather:
            return
        p = layer * 3 + mat
        for d in range(1, line):
            origin = lax.rem(z + line - d, line) * PAIR + x
            arrived(layer, mat, origin)
            block = slot(layer, mat, origin)
            go(remote(block, block, w_send_x.at[p, d], w_recv.at[p, origin], "sp", x_next))

    def settle(layer, mat):
        if not gather:
            return
        for d in range(line):
            arrived(layer, mat, lax.rem(z + line - d, line) * PAIR + (1 - x))

    def both_sides(make, count):
        for i in range(count):
            @pl.when(s > 0)
            def _():
                make(i, 0).start()

            @pl.when(s < n_sp - 1)
            def _():
                make(i, 1).start()

    def both_wait(make, count):
        for i in range(count):
            @pl.when(s > 0)
            def _():
                make(i, 0).wait_send()
                make(i, 1).wait_recv()

            @pl.when(s < n_sp - 1)
            def _():
                make(i, 1).wait_send()
                make(i, 0).wait_recv()

    def seg_copy(i, side):
        src = segw.at[pl.ds(fringe, fringe)] if side == 0 else segw.at[pl.ds(rows, fringe)]
        dst = segw.at[pl.ds(fringe + rows, fringe)] if side == 0 else segw.at[pl.ds(0, fringe)]
        return remote(src, dst, seg_send.at[side], seg_recv.at[side], "sp",
                      jnp.maximum(s - 1, 0) if side == 0 else jnp.minimum(s + 1, n_sp - 1))

    def halo_copy(layer):
        def make(i, side):
            buf = xbuf.at[layer, i]
            src = buf.at[pl.ds(fringe, fringe)] if side == 0 else buf.at[pl.ds(rows, fringe)]
            dst = buf.at[pl.ds(fringe + rows, fringe)] if side == 0 else buf.at[pl.ds(0, fringe)]
            return remote(src, dst, halo_send.at[layer, i, side], halo_recv.at[layer, i, side], "sp",
                          jnp.maximum(s - 1, 0) if side == 0 else jnp.minimum(s + 1, n_sp - 1))
        return make

    segw[pl.ds(fringe, rows)] = seg[...]

    @pl.when(s == 0)
    def _():
        segw[pl.ds(0, fringe)] = jnp.full((fringe, LANES), -1, jnp.int32)
        for layer in range(layers):
            for i in range(tiles):
                xbuf[layer, i, pl.ds(0, fringe)] = jnp.zeros((fringe, LANES), F32)

    @pl.when(s == n_sp - 1)
    def _():
        segw[pl.ds(fringe + rows, fringe)] = jnp.full((fringe, LANES), -1, jnp.int32)
        for layer in range(layers):
            for i in range(tiles):
                xbuf[layer, i, pl.ds(fringe + rows, fringe)] = jnp.zeros((fringe, LANES), F32)

    both_sides(seg_copy, 1)
    for mat in range(2):
        send_own(0, mat)
    for d in range(1, half):
        go(remote(tok, stream.at[0, t], tok_send.at[d], tok_recv.at[t], "tp", lax.rem(h + d, half) * PAIR + c))
    go(remote(tok, stream.at[0, t], sib_send.at[0, 0], tok_recv.at[t], "tp", sib))
    stream[0, t] = tok[...]
    relay(0, 0)
    send_own(0, 2)
    for d in range(1, half):
        origin = lax.rem(h + half - d, half) * PAIR + c
        block = stream.at[0, origin]
        remote(tok, block, tok_send.at[d], tok_recv.at[origin], "tp", sib).wait_recv()
        go(remote(block, block, sib_send.at[0, d], tok_recv.at[origin], "tp", sib))
    relay(0, 1)
    for d in range(half):
        origin = lax.rem(h + half - d, half) * PAIR + (1 - c)
        remote(tok, stream.at[0, origin], sib_send.at[0, d], tok_recv.at[origin], "tp", sib).wait_recv()
    both_wait(seg_copy, 1)

    for layer in range(layers):
        last = layer == layers - 1

        def norm_step(i, _):
            at = pl.ds(pl.multiple_of(i * 32, 32), 32)
            total = jnp.zeros((32, 1), F32)
            for j in range(n_tp):
                v = stream[layer, j, at, :].astype(F32)
                total = total + jnp.sum(v * v, axis=-1, keepdims=True)
            scale = lax.rsqrt(total / (n_tp * width) + EPSILON)
            for j in range(n_tp):
                v = stream[layer, j, at, :].astype(F32)
                cut = slice(j * width, (j + 1) * width)
                normed[at, cut] = (v * scale * gain_in[layer : layer + 1, cut]).astype(BF16)
            return 0

        lax.fori_loop(0, rows // 32, norm_step, 0)
        settle(layer, 0)
        settle(layer, 1)

        def gate_step(i):
            at = pl.ds(i * fringe, fringe)
            a = normed[at, :]
            if gather:
                w_value = gvg[layer, 0].reshape(n_tp * width, chan)
                w_gate = gvg[layer, 1].reshape(n_tp * width, chan)
            else:
                w_value, w_gate = wv[layer], wg[layer]
            value = jnp.dot(a, w_value, preferred_element_type=F32)
            gate = jnp.dot(a, w_gate, preferred_element_type=F32)
            gated = (value * jax.nn.sigmoid(gate)).astype(BF16).astype(F32)
            to = pl.ds(fringe + i * fringe, fringe)
            for j in range(tiles):
                xbuf[layer, j, to, :] = gated[:, j * LANES : (j + 1) * LANES]

        chunks = rows // fringe
        halo = halo_copy(layer)
        gate_step(0)
        gate_step(chunks - 1)
        both_sides(halo, tiles)
        if not last:
            send_own(layer + 1, 0)
        for i in range(1, chunks - 1):
            gate_step(i)

        def conv_step(i, _):
            base = pl.multiple_of(i * 32, 32)
            here = segw[pl.ds(base + fringe, 32), :]
            acc = [jnp.zeros((32, LANES), F32) for _ in range(tiles)]
            for k in range(kw):
                same = segw[pl.ds(base + k, 32), :] == here
                for j in range(tiles):
                    tap = taps[layer, k : k + 1, j * LANES : (j + 1) * LANES]
                    acc[j] = acc[j] + jnp.where(same, xbuf[layer, j, pl.ds(base + k, 32), :] * tap, 0.0)
            at = pl.ds(base, 32)
            total = sum(jnp.sum(a, axis=-1, keepdims=True) for a in acc)
            mean = total / chan
            square = sum(jnp.sum((a - mean) * (a - mean), axis=-1, keepdims=True) for a in acc)
            for j in range(tiles):
                conv[at, j * LANES : (j + 1) * LANES] = acc[j]
            lane = lax.broadcasted_iota(jnp.int32, (32, LANES), 1)
            part[at, :] = jnp.where(lane == 0, mean, square)
            return 0

        edge = fringe // 32
        lax.fori_loop(edge, rows // 32 - edge, conv_step, 0)
        relay(layer, 2)
        if not last:
            send_own(layer + 1, 1)
        both_wait(halo, tiles)
        lax.fori_loop(0, edge, conv_step, 0)
        lax.fori_loop(rows // 32 - edge, rows // 32, conv_step, 0)
        if not last:
            relay(layer + 1, 0)
            send_own(layer + 1, 2)

        stat[layer, t] = jnp.transpose(part[...])[:8]
        for d in range(1, n_tp):
            go(remote(stat.at[layer, t], stat.at[layer, t], stat_send.at[layer, d], stat_recv.at[layer, t], "tp", lax.rem(t + d, n_tp)))
        for d in range(1, n_tp):
            origin = lax.rem(t + n_tp - d, n_tp)
            remote(stat.at[layer, t], stat.at[layer, origin], stat_send.at[layer, d], stat_recv.at[layer, origin], "tp", origin).wait_recv()
        means = [stat[layer, j][0:1] for j in range(n_tp)]
        mean = sum(means) / n_tp
        spread = sum(stat[layer, j][1:2] + chan * (means[j] - mean) * (means[j] - mean) for j in range(n_tp))
        scale = lax.rsqrt(spread / (n_tp * chan) + EPSILON)
        row = lax.broadcasted_iota(jnp.int32, (LANES, rows), 0)
        part[...] = jnp.transpose(jnp.where(row == 0, mean, scale))

        def act_step(i, _):
            at = pl.ds(pl.multiple_of(i * 32, 32), 32)
            both = part[at, :]
            v = (conv[at, :] - both[:, 0:1]) * both[:, 1:2] * gain_norm[layer : layer + 1, :]
            act[at, :] = (v / (1.0 + jnp.exp(-v))).astype(BF16)
            return 0

        lax.fori_loop(0, rows // 32, act_step, 0)
        settle(layer, 2)

        blocks = gout if gather else wo
        cols = blocks.shape[-1]
        each = width // cols

        def project(target, put):
            for i in range(each):
                w = blocks[layer, target * each + i]
                put(slice(i * cols, (i + 1) * cols), jnp.dot(act[...], w, preferred_element_type=F32))

        for k in range(half):
            def put_first(cut, v, k=k):
                first[layer, 0, k, :, cut] = v.astype(BF16)

            project(k * PAIR + (1 - c), put_first)
            go(remote(first.at[layer, 0, k], first.at[layer, 1, k], first_send.at[layer, k], first_recv.at[layer, k], "tp", sib))
        for k in range(half):
            def put_own(cut, v, k=k):
                own[k, :, cut] = v

            project(k * PAIR + c, put_own)
        for d in range(half):
            k = lax.rem(h + half - 1 - d, half) if last else d
            remote(first.at[layer, 0, k], first.at[layer, 1, k], first_send.at[layer, k], first_recv.at[layer, k], "tp", sib).wait_recv()
            pair[layer, k] = (own[k] + first[layer, 1, k].astype(F32)).astype(BF16)
            if last:
                @pl.when(k != h)
                def _():
                    remote(pair.at[layer, k], far.at[layer, h, 0], fin_send.at[k], fin_recv.at[h], "tp", k * PAIR + c).start()
            else:
                for e in range(1, half):
                    go(remote(pair.at[layer, k], far.at[layer, h, k], far_send.at[layer, e, k], far_recv.at[layer, h, k], "tp",
                              lax.rem(h + e, half) * PAIR + c))
        if last:
            far[layer, h, 0] = pair[layer, h]
            for e in range(1, half):
                k = lax.rem(h + e, half)
                remote(pair.at[layer, k], far.at[layer, k, 0], fin_send.at[k], fin_recv.at[k], "tp", sib).wait()
            total = sum(far[layer, g, 0].astype(F32) for g in range(half))
            out[...] = (stream[layer, t].astype(F32) + total).astype(BF16)
        else:
            for k in range(half):
                far[layer, h, k] = pair[layer, k]
            relay(layer + 1, 1)
            for k in range(half):
                for e in range(1, half):
                    g = lax.rem(h + e, half)
                    remote(pair.at[layer, k], far.at[layer, g, k], far_send.at[layer, e, k], far_recv.at[layer, g, k], "tp", sib).wait_recv()
                total = sum(far[layer, g, k].astype(F32) for g in range(half))
                block = stream.at[layer + 1, k * PAIR + c]
                block[...] = (stream[layer, k * PAIR + c].astype(F32) + total).astype(BF16)
                go(remote(block, block, sib_send.at[layer + 1, k], far_recv.at[layer, half, k], "tp", sib))
            for k in range(half):
                block = stream.at[layer + 1, k * PAIR + (1 - c)]
                remote(block, block, sib_send.at[layer + 1, k], far_recv.at[layer, half, k], "tp", sib).wait_recv()

    for copy in sends:
        copy.wait_send()


def per_device(n_sp, n_tp, tokens, segments, in_gain, w_value, w_gate, conv_taps, norm_gain, w_out):
    layers, kw, chan = conv_taps.shape
    rows, width = tokens.shape
    gather = n_sp <= RELAY_MOST and n_sp % PAIR == 0
    if not gather:
        w_value = lax.all_gather(w_value, "sp", axis=1, tiled=True)
        w_gate = lax.all_gather(w_gate, "sp", axis=1, tiled=True)
        w_out = lax.all_gather(w_out, "sp", axis=2, tiled=True)
        w_out = w_out.reshape(layers, chan, n_tp, width).transpose(0, 2, 1, 3)
    held = (layers, 2, n_sp) + w_value.shape[1:] if gather else (1, 1, 1, 16, LANES)
    held_out = (layers, n_sp) + w_out.shape[1:] if gather else (1, 1, 16, LANES)
    tiles, half, fringe = chan // LANES, n_tp // PAIR, (kw - 1) // 2
    wide = rows + 2 * fringe
    dma = pltpu.SemaphoreType.DMA
    line = max(n_sp // PAIR, 1) if gather else 1
    held_sp = n_sp if gather else 1
    vmem = pl.BlockSpec(memory_space=pltpu.VMEM)
    return pl.pallas_call(
        functools.partial(kernel, (n_sp, n_tp, layers, kw, gather)),
        out_shape=jax.ShapeDtypeStruct((rows, width), BF16),
        in_specs=[vmem] * 8,
        out_specs=vmem,
        scratch_shapes=[
            pltpu.VMEM((layers, n_tp, rows, width), BF16),
            pltpu.VMEM((rows, n_tp * width), BF16),
            pltpu.VMEM(held, BF16),
            pltpu.VMEM(held_out, BF16),
            pltpu.VMEM((layers, tiles, wide, LANES), F32),
            pltpu.VMEM((wide, LANES), jnp.int32),
            pltpu.VMEM((rows, chan), F32),
            pltpu.VMEM((rows, chan), BF16),
            pltpu.VMEM((layers, n_tp, 8, rows), F32),
            pltpu.VMEM((rows, LANES), F32),
            pltpu.VMEM((layers, 2, half, rows, width), BF16),
            pltpu.VMEM((layers, half, rows, width), BF16),
            pltpu.VMEM((layers, half, half, rows, width), BF16),
            pltpu.VMEM((half, rows, width), F32),
            dma((layers * 3, held_sp)),
            dma((layers * 3, line)),
            dma((layers * 3, line)),
            dma((n_tp,)),
            dma((half,)),
            dma((layers, half)),
            dma((2,)),
            dma((2,)),
            dma((layers, tiles, 2)),
            dma((layers, tiles, 2)),
            dma((layers, n_tp)),
            dma((layers, n_tp)),
            dma((layers, half)),
            dma((layers, half)),
            dma((layers, half, half)),
            dma((layers, half + 1, half)),
            dma((half,)),
            dma((half,)),
        ],
        compiler_params=pltpu.CompilerParams(
            collective_id=0, has_side_effects=True, vmem_limit_bytes=60000 * 1024
        ),
    )(
        tokens,
        jnp.broadcast_to(segments[:, None], (rows, LANES)),
        in_gain,
        w_value,
        w_gate,
        w_out,
        conv_taps,
        norm_gain,
    )


def solution(mesh):
    in_specs = (
        P("sp", "tp"),
        P("sp"),
        P(),
        P(None, "sp", "tp"),
        P(None, "sp", "tp"),
        P(None, None, "tp"),
        P(None, "tp"),
        P(None, "tp", "sp"),
    )
    return jax.shard_map(
        functools.partial(per_device, mesh.shape["sp"], mesh.shape["tp"]),
        mesh=mesh,
        in_specs=in_specs,
        out_specs=P("sp", "tp"),
        check_vma=False,
    )
```

```python
import functools

import jax
import jax.numpy as jnp
from jax import lax
from jax.experimental import pallas as pl
from jax.experimental.pallas import tpu as pltpu
from jax.sharding import PartitionSpec as P

EPSILON = 0.01
LANES = 128
PAIR = 2
RELAY_MOST = 8
F32 = jnp.float32
BF16 = jnp.bfloat16
MESH = pl.DeviceIdType.MESH


def remote(src, dst, send, recv, axis, index):
    return pltpu.make_async_remote_copy(
        src_ref=src,
        dst_ref=dst,
        send_sem=send,
        recv_sem=recv,
        device_id={axis: index},
        device_id_type=MESH,
    )


def kernel(
    cfg, tok, seg, gain_in, wv, wg, wo, taps, gain_norm, out,
    stream, normed, gvg, gout, xbuf, segw, conv, act, stat, part, first, pair, far, own,
    w_recv, w_send_z, w_send_x, tok_recv, tok_send, sib_send, seg_send, seg_recv,
    halo_send, halo_recv, stat_send, stat_recv, first_send, first_recv,
    far_send, far_recv, fin_recv, fin_send,
):
    n_sp, n_tp, layers, kw, gather = cfg
    fringe = (kw - 1) // 2
    rows, width = tok.shape
    tiles = xbuf.shape[1]
    chan = tiles * LANES
    line, half = n_sp // PAIR, n_tp // PAIR
    s, t = lax.axis_index("sp"), lax.axis_index("tp")
    z, x = s // PAIR, lax.rem(s, PAIR)
    h, c = t // PAIR, lax.rem(t, PAIR)
    x_next = z * PAIR + (1 - x)
    sib = h * PAIR + (1 - c)

    barrier = pltpu.get_barrier_semaphore()
    greeted = range(1, n_sp) if gather else (1, n_sp - 1)
    for d in greeted:
        pl.semaphore_signal(barrier, inc=1, device_id={"sp": lax.rem(s + d, n_sp)}, device_id_type=MESH)
    for d in range(1, n_tp):
        pl.semaphore_signal(barrier, inc=1, device_id={"tp": lax.rem(t + d, n_tp)}, device_id_type=MESH)
    pl.semaphore_wait(barrier, len(greeted) + n_tp - 1)

    sends = []

    def go(copy):
        copy.start()
        sends.append(copy)

    def slot(layer, mat, origin):
        return gout.at[layer, origin] if mat == 2 else gvg.at[layer, mat, origin]

    def local(layer, mat):
        return (wv, wg, wo)[mat].at[layer]

    def send_own(layer, mat):
        if not gather:
            return
        p = layer * 3 + mat
        for d in range(1, line):
            go(remote(local(layer, mat), slot(layer, mat, s), w_send_z.at[p, d], w_recv.at[p, s], "sp",
                      lax.rem(z + d, line) * PAIR + x))
        go(remote(local(layer, mat), slot(layer, mat, s), w_send_x.at[p, 0], w_recv.at[p, s], "sp", x_next))
        slot(layer, mat, s)[...] = local(layer, mat)[...]

    def arrived(layer, mat, origin):
        p = layer * 3 + mat
        remote(local(layer, mat), slot(layer, mat, origin), w_send_x.at[p, 0], w_recv.at[p, origin], "sp", x_next).wait_recv()

    def relay(layer, mat):
        if not gather:
            return
        p = layer * 3 + mat
        for d in range(1, line):
            origin = lax.rem(z + line - d, line) * PAIR + x
            arrived(layer, mat, origin)
            block = slot(layer, mat, origin)
            go(remote(block, block, w_send_x.at[p, d], w_recv.at[p, origin], "sp", x_next))

    def settle(layer, mat):
        if not gather:
            return
        for d in range(line):
            arrived(layer, mat, lax.rem(z + line - d, line) * PAIR + (1 - x))

    def both_sides(make, count):
        for i in range(count):
            @pl.when(s > 0)
            def _():
                make(i, 0).start()

            @pl.when(s < n_sp - 1)
            def _():
                make(i, 1).start()

    def both_wait(make, count):
        for i in range(count):
            @pl.when(s > 0)
            def _():
                make(i, 0).wait_send()
                make(i, 1).wait_recv()

            @pl.when(s < n_sp - 1)
            def _():
                make(i, 1).wait_send()
                make(i, 0).wait_recv()

    def seg_copy(i, side):
        src = segw.at[pl.ds(fringe, fringe)] if side == 0 else segw.at[pl.ds(rows, fringe)]
        dst = segw.at[pl.ds(fringe + rows, fringe)] if side == 0 else segw.at[pl.ds(0, fringe)]
        return remote(src, dst, seg_send.at[side], seg_recv.at[side], "sp",
                      jnp.maximum(s - 1, 0) if side == 0 else jnp.minimum(s + 1, n_sp - 1))

    def halo_copy(layer):
        def make(i, side):
            buf = xbuf.at[layer, i]
            src = buf.at[pl.ds(fringe, fringe)] if side == 0 else buf.at[pl.ds(rows, fringe)]
            dst = buf.at[pl.ds(fringe + rows, fringe)] if side == 0 else buf.at[pl.ds(0, fringe)]
            return remote(src, dst, halo_send.at[layer, i, side], halo_recv.at[layer, i, side], "sp",
                          jnp.maximum(s - 1, 0) if side == 0 else jnp.minimum(s + 1, n_sp - 1))
        return make

    segw[pl.ds(fringe, rows)] = seg[...]

    @pl.when(s == 0)
    def _():
        segw[pl.ds(0, fringe)] = jnp.full((fringe, LANES), -1, jnp.int32)
        for layer in range(layers):
            for i in range(tiles):
                xbuf[layer, i, pl.ds(0, fringe)] = jnp.zeros((fringe, LANES), F32)

    @pl.when(s == n_sp - 1)
    def _():
        segw[pl.ds(fringe + rows, fringe)] = jnp.full((fringe, LANES), -1, jnp.int32)
        for layer in range(layers):
            for i in range(tiles):
                xbuf[layer, i, pl.ds(fringe + rows, fringe)] = jnp.zeros((fringe, LANES), F32)

    both_sides(seg_copy, 1)
    for mat in range(2):
        send_own(0, mat)
    for d in range(1, half):
        go(remote(tok, stream.at[0, t], tok_send.at[d], tok_recv.at[t], "tp", lax.rem(h + d, half) * PAIR + c))
    go(remote(tok, stream.at[0, t], sib_send.at[0, 0], tok_recv.at[t], "tp", sib))
    stream[0, t] = tok[...]
    relay(0, 0)
    send_own(0, 2)
    for d in range(1, half):
        origin = lax.rem(h + half - d, half) * PAIR + c
        block = stream.at[0, origin]
        remote(tok, block, tok_send.at[d], tok_recv.at[origin], "tp", sib).wait_recv()
        go(remote(block, block, sib_send.at[0, d], tok_recv.at[origin], "tp", sib))
    relay(0, 1)
    for d in range(half):
        origin = lax.rem(h + half - d, half) * PAIR + (1 - c)
        remote(tok, stream.at[0, origin], sib_send.at[0, d], tok_recv.at[origin], "tp", sib).wait_recv()
    both_wait(seg_copy, 1)

    for layer in range(layers):
        last = layer == layers - 1

        def norm_step(i, _):
            at = pl.ds(pl.multiple_of(i * 32, 32), 32)
            total = jnp.zeros((32, 1), F32)
            for j in range(n_tp):
                v = stream[layer, j, at, :].astype(F32)
                total = total + jnp.sum(v * v, axis=-1, keepdims=True)
            scale = lax.rsqrt(total / (n_tp * width) + EPSILON)
            for j in range(n_tp):
                v = stream[layer, j, at, :].astype(F32)
                cut = slice(j * width, (j + 1) * width)
                normed[at, cut] = (v * scale * gain_in[layer : layer + 1, cut]).astype(BF16)
            return 0

        lax.fori_loop(0, rows // 32, norm_step, 0)
        settle(layer, 0)
        settle(layer, 1)

        def gate_step(i):
            at = pl.ds(i * fringe, fringe)
            a = normed[at, :]
            if gather:
                w_value = gvg[layer, 0].reshape(n_tp * width, chan)
                w_gate = gvg[layer, 1].reshape(n_tp * width, chan)
            else:
                w_value, w_gate = wv[layer], wg[layer]
            value = jnp.dot(a, w_value, preferred_element_type=F32)
            gate = jnp.dot(a, w_gate, preferred_element_type=F32)
            gated = (value * jax.nn.sigmoid(gate)).astype(BF16).astype(F32)
            to = pl.ds(fringe + i * fringe, fringe)
            for j in range(tiles):
                xbuf[layer, j, to, :] = gated[:, j * LANES : (j + 1) * LANES]

        chunks = rows // fringe
        halo = halo_copy(layer)
        gate_step(0)
        gate_step(chunks - 1)
        both_sides(halo, tiles)
        if not last:
            send_own(layer + 1, 0)
        for i in range(1, chunks - 1):
            gate_step(i)

        def conv_step(i, _):
            base = pl.multiple_of(i * 32, 32)
            here = segw[pl.ds(base + fringe, 32), :]
            acc = [jnp.zeros((32, LANES), F32) for _ in range(tiles)]
            for shift in range(8):
                reach = (kw - 1 - shift) // 8 * 8
                docs = segw[pl.ds(base + shift, 32 + reach), :]
                data = [xbuf[layer, j, pl.ds(base + shift, 32 + reach), :] for j in range(tiles)]
                for q in range(0, reach + 1, 8):
                    same, k = docs[q : q + 32] == here, q + shift
                    for j in range(tiles):
                        tap = taps[layer, k : k + 1, j * LANES : (j + 1) * LANES]
                        acc[j] = acc[j] + jnp.where(same, data[j][q : q + 32] * tap, 0.0)
            at = pl.ds(base, 32)
            total = sum(jnp.sum(a, axis=-1, keepdims=True) for a in acc)
            mean = total / chan
            square = sum(jnp.sum((a - mean) * (a - mean), axis=-1, keepdims=True) for a in acc)
            for j in range(tiles):
                conv[at, j * LANES : (j + 1) * LANES] = acc[j]
            lane = lax.broadcasted_iota(jnp.int32, (32, LANES), 1)
            part[at, :] = jnp.where(lane == 0, mean, square)
            return 0

        edge = fringe // 32
        lax.fori_loop(edge, rows // 32 - edge, conv_step, 0)
        relay(layer, 2)
        if not last:
            send_own(layer + 1, 1)
        both_wait(halo, tiles)
        lax.fori_loop(0, edge, conv_step, 0)
        lax.fori_loop(rows // 32 - edge, rows // 32, conv_step, 0)
        if not last:
            send_own(layer + 1, 2)

        stat[layer, t] = jnp.transpose(part[...])[:8]
        for d in range(1, n_tp):
            go(remote(stat.at[layer, t], stat.at[layer, t], stat_send.at[layer, d], stat_recv.at[layer, t], "tp", lax.rem(t + d, n_tp)))
        for d in range(1, n_tp):
            origin = lax.rem(t + n_tp - d, n_tp)
            remote(stat.at[layer, t], stat.at[layer, origin], stat_send.at[layer, d], stat_recv.at[layer, origin], "tp", origin).wait_recv()
        means = [stat[layer, j][0:1] for j in range(n_tp)]
        mean = sum(means) / n_tp
        spread = sum(stat[layer, j][1:2] + chan * (means[j] - mean) * (means[j] - mean) for j in range(n_tp))
        scale = lax.rsqrt(spread / (n_tp * chan) + EPSILON)
        row = lax.broadcasted_iota(jnp.int32, (LANES, rows), 0)
        part[...] = jnp.transpose(jnp.where(row == 0, mean, scale))

        def act_step(i, _):
            at = pl.ds(pl.multiple_of(i * 32, 32), 32)
            both = part[at, :]
            v = (conv[at, :] - both[:, 0:1]) * both[:, 1:2] * gain_norm[layer : layer + 1, :]
            act[at, :] = (v / (1.0 + jnp.exp(-v))).astype(BF16)
            return 0

        lax.fori_loop(0, rows // 32, act_step, 0)
        settle(layer, 2)

        blocks = gout if gather else wo
        cols = blocks.shape[-1]
        each = width // cols

        def project(target, put):
            for i in range(each):
                w = blocks[layer, target * each + i]
                put(slice(i * cols, (i + 1) * cols), jnp.dot(act[...], w, preferred_element_type=F32))

        for k in range(half):
            def put_first(cut, v, k=k):
                first[layer, 0, k, :, cut] = v.astype(BF16)

            project(k * PAIR + (1 - c), put_first)
            go(remote(first.at[layer, 0, k], first.at[layer, 1, k], first_send.at[layer, k], first_recv.at[layer, k], "tp", sib))
        if not last:
            relay(layer + 1, 0)
        for k in range(half):
            def put_own(cut, v, k=k):
                own[k, :, cut] = v

            project(k * PAIR + c, put_own)
        for d in range(half):
            k = lax.rem(h + half - 1 - d, half) if last else d
            remote(first.at[layer, 0, k], first.at[layer, 1, k], first_send.at[layer, k], first_recv.at[layer, k], "tp", sib).wait_recv()
            pair[layer, k] = (own[k] + first[layer, 1, k].astype(F32)).astype(BF16)
            if last:
                @pl.when(k != h)
                def _():
                    remote(pair.at[layer, k], far.at[layer, h, 0], fin_send.at[k], fin_recv.at[h], "tp", k * PAIR + c).start()
            else:
                for e in range(1, half):
                    go(remote(pair.at[layer, k], far.at[layer, h, k], far_send.at[layer, e, k], far_recv.at[layer, h, k], "tp",
                              lax.rem(h + e, half) * PAIR + c))
        if last:
            far[layer, h, 0] = pair[layer, h]
            for e in range(1, half):
                k = lax.rem(h + e, half)
                remote(pair.at[layer, k], far.at[layer, k, 0], fin_send.at[k], fin_recv.at[k], "tp", sib).wait()
            total = sum(far[layer, g, 0].astype(F32) for g in range(half))
            out[...] = (stream[layer, t].astype(F32) + total).astype(BF16)
        else:
            for k in range(half):
                far[layer, h, k] = pair[layer, k]
            relay(layer + 1, 1)
            for k in range(half):
                for e in range(1, half):
                    g = lax.rem(h + e, half)
                    remote(pair.at[layer, k], far.at[layer, g, k], far_send.at[layer, e, k], far_recv.at[layer, g, k], "tp", sib).wait_recv()
                total = sum(far[layer, g, k].astype(F32) for g in range(half))
                block = stream.at[layer + 1, k * PAIR + c]
                block[...] = (stream[layer, k * PAIR + c].astype(F32) + total).astype(BF16)
                go(remote(block, block, sib_send.at[layer + 1, k], far_recv.at[layer, half, k], "tp", sib))
            for k in range(half):
                block = stream.at[layer + 1, k * PAIR + (1 - c)]
                remote(block, block, sib_send.at[layer + 1, k], far_recv.at[layer, half, k], "tp", sib).wait_recv()

    for copy in sends:
        copy.wait_send()


def per_device(n_sp, n_tp, tokens, segments, in_gain, w_value, w_gate, conv_taps, norm_gain, w_out):
    layers, kw, chan = conv_taps.shape
    rows, width = tokens.shape
    gather = n_sp <= RELAY_MOST and n_sp % PAIR == 0
    if not gather:
        w_value = lax.all_gather(w_value, "sp", axis=1, tiled=True)
        w_gate = lax.all_gather(w_gate, "sp", axis=1, tiled=True)
        w_out = lax.all_gather(w_out, "sp", axis=2, tiled=True)
        w_out = w_out.reshape(layers, chan, n_tp, width).transpose(0, 2, 1, 3)
    held = (layers, 2, n_sp) + w_value.shape[1:] if gather else (1, 1, 1, 16, LANES)
    held_out = (layers, n_sp) + w_out.shape[1:] if gather else (1, 1, 16, LANES)
    tiles, half, fringe = chan // LANES, n_tp // PAIR, (kw - 1) // 2
    wide = rows + 2 * fringe
    dma = pltpu.SemaphoreType.DMA
    line = max(n_sp // PAIR, 1) if gather else 1
    held_sp = n_sp if gather else 1
    vmem = pl.BlockSpec(memory_space=pltpu.VMEM)
    return pl.pallas_call(
        functools.partial(kernel, (n_sp, n_tp, layers, kw, gather)),
        out_shape=jax.ShapeDtypeStruct((rows, width), BF16),
        in_specs=[vmem] * 8,
        out_specs=vmem,
        scratch_shapes=[
            pltpu.VMEM((layers, n_tp, rows, width), BF16),
            pltpu.VMEM((rows, n_tp * width), BF16),
            pltpu.VMEM(held, BF16),
            pltpu.VMEM(held_out, BF16),
            pltpu.VMEM((layers, tiles, wide, LANES), F32),
            pltpu.VMEM((wide, LANES), jnp.int32),
            pltpu.VMEM((rows, chan), F32),
            pltpu.VMEM((rows, chan), BF16),
            pltpu.VMEM((layers, n_tp, 8, rows), F32),
            pltpu.VMEM((rows, LANES), F32),
            pltpu.VMEM((layers, 2, half, rows, width), BF16),
            pltpu.VMEM((layers, half, rows, width), BF16),
            pltpu.VMEM((layers, half, half, rows, width), BF16),
            pltpu.VMEM((half, rows, width), F32),
            dma((layers * 3, held_sp)),
            dma((layers * 3, line)),
            dma((layers * 3, line)),
            dma((n_tp,)),
            dma((half,)),
            dma((layers, half)),
            dma((2,)),
            dma((2,)),
            dma((layers, tiles, 2)),
            dma((layers, tiles, 2)),
            dma((layers, n_tp)),
            dma((layers, n_tp)),
            dma((layers, half)),
            dma((layers, half)),
            dma((layers, half, half)),
            dma((layers, half + 1, half)),
            dma((half,)),
            dma((half,)),
        ],
        compiler_params=pltpu.CompilerParams(
            collective_id=0, has_side_effects=True, vmem_limit_bytes=60000 * 1024
        ),
    )(
        tokens,
        jnp.broadcast_to(segments[:, None], (rows, LANES)),
        in_gain,
        w_value,
        w_gate,
        w_out,
        conv_taps,
        norm_gain,
    )


def solution(mesh):
    in_specs = (
        P("sp", "tp"),
        P("sp"),
        P(),
        P(None, "sp", "tp"),
        P(None, "sp", "tp"),
        P(None, None, "tp"),
        P(None, "tp"),
        P(None, "tp", "sp"),
    )
    return jax.shard_map(
        functools.partial(per_device, mesh.shape["sp"], mesh.shape["tp"]),
        mesh=mesh,
        in_specs=in_specs,
        out_specs=P("sp", "tp"),
        check_vma=False,
    )
```
